32 devices in a mesh: kv: 8 (over z, y), tp: 4 (over x, core).
Axes of the slice: x: 2, y: 2, z: 4, core: 2. Of those that a mesh axis runs over, the one named last changes fastest.
Arguments:
- tokens: bfloat16 [32, 4096], P(None, ('kv', 'tp')), may hold values from -12 to 12
- first_gain: bfloat16 [4096], replicated, may hold values from 0.099609375 to 1.8984375
- first_gate: bfloat16 [4096, 11264], P(None, ('kv', 'tp')), may hold values from -0.09375 to 0.09375
- first_up: bfloat16 [4096, 11264], P(None, ('kv', 'tp')), may hold values from -0.09375 to 0.09375
- first_down: bfloat16 [11264, 4096], P(('kv', 'tp')), may hold values from -0.109375 to 0.109375
- mix_gain: bfloat16 [4096], replicated, may hold values from 0.099609375 to 1.8984375
- query_weight: bfloat16 [4096, 1024], P('kv', 'tp'), may hold values from -0.09375 to 0.09375
- key_weight: bfloat16 [4096, 1024], P('kv', 'tp'), may hold values from -0.09375 to 0.09375
- value_weight: bfloat16 [4096, 2048], P('kv', 'tp'), may hold values from -0.09375 to 0.09375
- outgate_weight: bfloat16 [4096, 2048], P('kv', 'tp'), may hold values from -0.09375 to 0.09375
- ingate_weight: bfloat16 [4096, 8], P('kv'), may hold values from -0.09375 to 0.09375
- forget_weight: bfloat16 [4096, 8], P('kv'), may hold values from -0.09375 to 0.09375
- forget_bias: float32 [8], P('tp'), may hold values from -1 to 4
- head_gain: bfloat16 [2048], P('tp'), may hold values from 0.099609375 to 1.8984375
- mixout_weight: bfloat16 [2048, 4096], P('tp', 'kv'), may hold values from -0.125 to 0.125
- memory: float32 [32, 8, 128, 256], P('kv', 'tp'), may hold values from -0.6 to 0.6
- stabilizer: float32 [32, 8], P('kv', 'tp'), may hold values from -4 to 4
- second_gain: bfloat16 [4096], replicated, may hold values from 0.099609375 to 1.8984375
- second_gate: bfloat16 [4096, 11264], P(None, ('kv', 'tp')), may hold values from -0.09375 to 0.09375
- second_up: bfloat16 [4096, 11264], P(None, ('kv', 'tp')), may hold values from -0.09375 to 0.09375
- second_down: bfloat16 [11264, 4096], P(('kv', 'tp')), may hold values from -0.109375 to 0.109375
Outputs:
- layer_out: bfloat16 [32, 4096], P(None, ('kv', 'tp'))
- memory_next: float32 [32, 8, 128, 256], P('kv', 'tp')
- stabilizer_next: float32 [32, 8], P('kv', 'tp')
The draws below stay inside these ranges and needn't reach their ends.
All inputs are finite; a program needn't handle non-finite values.
Results may differ from the reference program's by a relative error of at most 0.013.
Values may be sent and summed in bfloat16 or wider, within the bound.
A program may use at most 64 MiB of HBM per device.

```python
import jax
import jax.numpy as jnp
from jax import lax

D = 4096
FF = 11264
H = 8
DK = 128
DV = 256
BATCH = 32


def draw_tokens(key, part):
    column = jnp.arange(D, dtype=jnp.float32)
    ramp = 0.5 * 4.0 ** (column / D)
    values = jax.random.normal(key, (BATCH, D), jnp.float32) * ramp[None, :]
    return jnp.clip(values, -12.0, 12.0).astype(jnp.bfloat16)


def with_spikes(result, key, source, target, parts, factor):
    owner, partner = [(jnp.arange(result.shape[position]) // (result.shape[position] // parts)).reshape([-1 if axis == position else 1 for axis in range(result.ndim)]) for position in (source, target)]
    chosen = jax.random.permutation(key, parts)[partner]
    strong = (owner == chosen) | (owner == (partner + parts // 2) % parts)
    return jnp.where(strong, factor * result, result)


def steps_of(key, shape, cuts, smallest, high):
    factor_of = 1.0
    for position, shards_of in cuts:
        steps = jax.random.uniform(jax.random.fold_in(jax.random.fold_in(key, 6), position), (shards_of,), jnp.float32, smallest / len(cuts), high / len(cuts))
        factor_of = factor_of * jnp.repeat(jnp.exp(steps), shape[position] // shards_of).reshape((-1,) + (1,) * (len(shape) - 1 - position))
    return factor_of


def gaussian(key, dims, spread, reach, cuts=(), kind=jnp.bfloat16):
    drawn = spread * jax.random.normal(key, dims, jnp.float32)
    if cuts:
        drawn = drawn * steps_of(key, dims, cuts, -0.22, 0.18)
    return jnp.clip(drawn, -reach, reach).astype(kind)


def bell_draw_with(key, extent, scale, most, shards, heavy, held_as=jnp.bfloat16):
    entries = scale * jax.random.normal(key, extent, jnp.float32)
    if shards:
        entries = entries * steps_of(key, extent, shards, -0.22, 0.18)
    return jnp.clip(with_spikes(entries, jax.random.fold_in(key, 3), *heavy), -most, most).astype(held_as)


def setup_inputs(seed: int = 0) -> dict:
    seeds = jax.random.split(jax.random.key(seed), 22)
    tokens = draw_tokens(jax.random.fold_in(seeds[21], 71), 0)
    first_gain = jnp.clip(1.0 + 0.18 * jax.random.normal(seeds[1], (D,), jnp.float32), 0.099609375, 1.8984375).astype(jnp.bfloat16)
    first_gate = gaussian(seeds[2], (D, FF), D ** -0.5, 0.09375, ((1, 32),))
    first_up = gaussian(seeds[3], (D, FF), D ** -0.5, 0.09375, ((1, 32),))
    first_down = bell_draw_with(seeds[4], (FF, D), FF ** -0.5, 0.109375, ((0, 32),), (0, 1, 32, 2.75))
    mix_gain = jnp.clip(1.0 + 0.18 * jax.random.normal(seeds[5], (D,), jnp.float32), 0.099609375, 1.8984375).astype(jnp.bfloat16)
    query_weight = gaussian(seeds[6], (D, H * DK), D ** -0.5, 0.09375, ((0, 8), (1, 4)))
    key_weight = gaussian(seeds[7], (D, H * DK), D ** -0.5, 0.09375, ((0, 8), (1, 4)))
    value_weight = gaussian(seeds[8], (D, H * DV), D ** -0.5, 0.09375, ((0, 8), (1, 4)))
    outgate_weight = gaussian(seeds[9], (D, H * DV), D ** -0.5, 0.09375, ((0, 8), (1, 4)))
    ingate_weight = gaussian(seeds[10], (D, H), D ** -0.5, 0.09375, ((0, 8),))
    forget_weight = gaussian(seeds[11], (D, H), D ** -0.5, 0.09375, ((0, 8),))
    forget_bias = jnp.clip(-1.0 + 5.0 * jax.random.uniform(seeds[12], (H,), jnp.float32) ** steps_of(seeds[12], (H,), ((0, 4),), -0.2, 0.2), -1.0, 4.0)
    head_gain = jnp.clip(1.0 + 0.18 * jax.random.normal(seeds[13], (H * DV,), jnp.float32), 0.099609375, 1.8984375).astype(jnp.bfloat16)
    mixout_weight = gaussian(seeds[14], (H * DV, D), (H * DV) ** -0.5, 0.125, ((0, 4), (1, 8)))
    memory = gaussian(seeds[15], (BATCH, H, DK, DV), 0.1, 0.6, ((0, 8), (1, 4)), jnp.float32)
    stabilizer = gaussian(seeds[16], (BATCH, H), 1.0, 4.0, ((0, 8), (1, 4)), jnp.float32)
    second_gain = jnp.clip(1.0 + 0.18 * jax.random.normal(seeds[17], (D,), jnp.float32), 0.099609375, 1.8984375).astype(jnp.bfloat16)
    second_gate = gaussian(seeds[18], (D, FF), D ** -0.5, 0.09375, ((1, 32),))
    second_up = gaussian(seeds[19], (D, FF), D ** -0.5, 0.09375, ((1, 32),))
    second_down = bell_draw_with(seeds[20], (FF, D), FF ** -0.5, 0.109375, ((0, 32),), (0, 1, 32, 2.75))
    return dict(tokens=tokens, first_gain=first_gain, first_gate=first_gate, first_up=first_up, first_down=first_down, mix_gain=mix_gain, query_weight=query_weight, key_weight=key_weight, value_weight=value_weight, outgate_weight=outgate_weight, ingate_weight=ingate_weight, forget_weight=forget_weight, forget_bias=forget_bias, head_gain=head_gain, mixout_weight=mixout_weight, memory=memory, stabilizer=stabilizer, second_gain=second_gain, second_gate=second_gate, second_up=second_up, second_down=second_down)


epsilon = 1e-06

def row_scale(wide_values):
    return lax.rsqrt(lax.optimization_barrier(jnp.mean(wide_values * wide_values, axis=-1, keepdims=True)) + epsilon)

def half_mlp(tokens, norm_gain, gate_weight, up_weight, down_weight):
    wide_tokens = tokens.astype(jnp.float32)
    row_factor = row_scale(wide_tokens)
    normed = (wide_tokens * norm_gain.astype(jnp.float32)).astype(jnp.bfloat16)
    gate_sum = row_factor * jnp.dot(normed, gate_weight, preferred_element_type=jnp.float32)
    up_sum = row_factor * jnp.dot(normed, up_weight, preferred_element_type=jnp.float32)
    hidden = (jax.nn.silu(gate_sum) * up_sum).astype(jnp.bfloat16)
    branch = jnp.dot(hidden, down_weight, preferred_element_type=jnp.float32)
    return (wide_tokens + 0.5 * branch).astype(jnp.bfloat16)

def reference(tokens, first_gain, first_gate, first_up, first_down, mix_gain, query_weight, key_weight, value_weight, outgate_weight, ingate_weight, forget_weight, forget_bias, head_gain, mixout_weight, memory, stabilizer, second_gain, second_gate, second_up, second_down):
    first = half_mlp(tokens, first_gain, first_gate, first_up, first_down)
    wide_first = first.astype(jnp.float32)
    row_factor = row_scale(wide_first)
    normed = (wide_first * mix_gain.astype(jnp.float32)).astype(jnp.bfloat16)
    rows_total = tokens.shape[0]

    def project(matrix):
        return row_factor * jnp.dot(normed, matrix, preferred_element_type=jnp.float32)
    query = project(query_weight).astype(jnp.bfloat16).reshape(rows_total, H, DK)
    keys = project(key_weight).astype(jnp.bfloat16).reshape(rows_total, H, DK)
    values = project(value_weight).astype(jnp.bfloat16).reshape(rows_total, H, DV)
    outgate = project(outgate_weight).astype(jnp.bfloat16).reshape(rows_total, H, DV)
    ingate = project(ingate_weight)
    forget = project(forget_weight) + forget_bias[None, :]
    log_forget = jax.nn.log_sigmoid(forget)
    ceiling = jnp.maximum(log_forget + stabilizer, ingate)
    retain = jnp.exp(log_forget + stabilizer - ceiling)
    admission = jnp.exp(ingate - ceiling)
    scaled_keys = keys.astype(jnp.float32) * DK ** (-0.5)
    outer_product = jnp.einsum('bhd,bhe->bhde', scaled_keys, values.astype(jnp.float32))
    memory_next = retain[..., None, None] * memory + admission[..., None, None] * outer_product
    readout = jnp.einsum('bhd,bhde->bhe', query.astype(jnp.float32), memory_next, precision=lax.Precision.HIGHEST)
    normalized = readout * lax.rsqrt(lax.optimization_barrier(jnp.mean(readout * readout, axis=-1, keepdims=True)) + epsilon)
    gated = normalized * head_gain.reshape(H, DV).astype(jnp.float32) * jax.nn.sigmoid(outgate.astype(jnp.float32))
    mixed = gated.reshape(rows_total, H * DV).astype(jnp.bfloat16)
    mix_branch = jnp.dot(mixed, mixout_weight, preferred_element_type=jnp.float32)
    after_mix = (wide_first + mix_branch).astype(jnp.bfloat16)
    layer_out = half_mlp(after_mix, second_gain, second_gate, second_up, second_down)
    return (layer_out, memory_next, ceiling)
```

```python
import functools

import jax
import jax.numpy as jnp
from jax import lax
from jax.experimental import pallas as pl
from jax.experimental.pallas import tpu as pltpu
from jax.sharding import PartitionSpec as P

epsilon = 1e-06


def row_scale(squares, model_width):
    return lax.rsqrt(squares / model_width + epsilon)[:, None]


def fold_columns(column_block, gain_vector, matrices):
    wide_block = column_block.astype(jnp.float32)
    gain_piece = gain_vector.astype(jnp.float32)
    normed = (wide_block * gain_piece).astype(jnp.bfloat16)
    updated = tuple(
        (jnp.dot(normed, matrix, preferred_element_type=jnp.float32) for matrix in matrices)
    )
    return (updated, jnp.sum(wide_block * wide_block, axis=1))


def half_mlp(tokens, norm_gain, gate_weight, up_weight, down_weight):
    model_width = norm_gain.shape[0]
    (gate_sum, up_sum), squares = fold_columns(
        lax.all_gather(tokens, ("kv", "tp"), axis=1, tiled=True),
        norm_gain,
        (gate_weight, up_weight),
    )
    row_factor = row_scale(squares, model_width)
    hidden = (jax.nn.silu(row_factor * gate_sum) * (row_factor * up_sum)).astype(jnp.bfloat16)
    branch = lax.psum_scatter(
        lax.dot_general(
            down_weight, hidden, (((0,), (1,)), ((), ())), preferred_element_type=jnp.float32
        ),
        ("kv", "tp"),
        scatter_dimension=0,
        tiled=True,
    ).T
    return (tokens.astype(jnp.float32) + 0.5 * branch).astype(jnp.bfloat16)


def on_device(
    tokens,
    first_gain,
    first_gate,
    first_up,
    first_down,
    mix_gain,
    query_weight,
    key_weight,
    value_weight,
    outgate_weight,
    ingate_weight,
    forget_weight,
    forget_bias,
    head_gain,
    mixout_weight,
    memory,
    stabilizer,
    second_gain,
    second_gate,
    second_up,
    second_down,
):
    first = half_mlp(tokens, first_gain, first_gate, first_up, first_down)
    matrices = (
        query_weight,
        key_weight,
        value_weight,
        outgate_weight,
        ingate_weight,
        forget_weight,
    )
    block_width = query_weight.shape[0]
    gain_block = lax.dynamic_slice_in_dim(
        mix_gain, lax.axis_index("kv") * block_width, block_width, 0
    )
    mix_partials, squares = fold_columns(
        lax.all_gather(first, "tp", axis=1, tiled=True), gain_block, matrices
    )
    query_sum, key_sum, value_sum, outgate_sum, ingate_sum, forget_sum, squares = (
        lax.psum_scatter(mix_partials[0], "kv", scatter_dimension=0, tiled=True),
        lax.psum_scatter(mix_partials[1], "kv", scatter_dimension=0, tiled=True),
        lax.psum_scatter(mix_partials[2], "kv", scatter_dimension=0, tiled=True),
        lax.psum_scatter(mix_partials[3], "kv", scatter_dimension=0, tiled=True),
        lax.psum_scatter(mix_partials[4], "kv", scatter_dimension=0, tiled=True),
        lax.psum_scatter(mix_partials[5], "kv", scatter_dimension=0, tiled=True),
        lax.psum_scatter(squares, "kv", scatter_dimension=0, tiled=True),
    )
    row_factor = row_scale(squares, mix_gain.shape[0])
    seq_local, heads_local, key_width, value_width = memory.shape
    query = (row_factor * query_sum).astype(jnp.bfloat16).reshape(seq_local, heads_local, key_width)
    keys = (row_factor * key_sum).astype(jnp.bfloat16).reshape(seq_local, heads_local, key_width)
    values = (
        (row_factor * value_sum).astype(jnp.bfloat16).reshape(seq_local, heads_local, value_width)
    )
    outgate = (
        (row_factor * outgate_sum).astype(jnp.bfloat16).reshape(seq_local, heads_local, value_width)
    )
    head_start = lax.axis_index("tp") * heads_local
    ingate = lax.dynamic_slice_in_dim(row_factor * ingate_sum, head_start, heads_local, 1)
    forget = (
        lax.dynamic_slice_in_dim(row_factor * forget_sum, head_start, heads_local, 1)
        + forget_bias[None, :]
    )
    log_forget = jax.nn.log_sigmoid(forget)
    ceiling = jnp.maximum(log_forget + stabilizer, ingate)
    retain = jnp.exp(log_forget + stabilizer - ceiling)
    admission = jnp.exp(ingate - ceiling)
    scaled_keys = keys.astype(jnp.float32) * key_width ** (-0.5)
    outer_product = jnp.einsum("shd,she->shde", scaled_keys, values.astype(jnp.float32))
    memory_next = retain[..., None, None] * memory + admission[..., None, None] * outer_product
    readout = jnp.einsum(
        "shd,shde->she", query.astype(jnp.float32), memory_next, precision=lax.Precision.HIGHEST
    )
    normalized = readout * lax.rsqrt(jnp.mean(readout * readout, axis=-1, keepdims=True) + epsilon)
    gated = (
        normalized
        * head_gain.reshape(heads_local, value_width).astype(jnp.float32)
        * jax.nn.sigmoid(outgate.astype(jnp.float32))
    )
    mixed = gated.reshape(seq_local, heads_local * value_width).astype(jnp.bfloat16)
    mix_terms = jnp.dot(
        lax.all_gather(mixed, "kv", axis=0, tiled=True),
        mixout_weight,
        preferred_element_type=jnp.float32,
    )
    mix_branch = lax.psum_scatter(
        mix_terms.astype(jnp.bfloat16), "tp", scatter_dimension=1, tiled=True
    ).astype(jnp.float32)
    after_mix = (first.astype(jnp.float32) + mix_branch).astype(jnp.bfloat16)
    layer_out = half_mlp(after_mix, second_gain, second_gate, second_up, second_down)
    return (layer_out, memory_next, ceiling)


def fused_kernel(
    kv_count,
    tp_count,
    tokens,
    first_gain,
    mix_gain,
    second_gain,
    head_gain,
    forget_bias,
    stabilizer,
    first_gate,
    first_up,
    first_down,
    query_weight,
    key_weight,
    value_weight,
    outgate_weight,
    ingate_weight,
    forget_weight,
    mixout_weight,
    memory,
    second_gate,
    second_up,
    second_down,
    layer_out,
    memory_next,
    ceiling_out,
    gate_a,
    up_a,
    down_a,
    gate_b,
    up_b,
    down_b,
    query_w,
    key_w,
    value_w,
    outgate_w,
    ingate_w,
    forget_w,
    mixout_w,
    memory_v,
    gathered_a,
    parts_a,
    landed_a,
    gathered_b,
    parts_b,
    landed_b,
    first_v,
    block_v,
    proj_send,
    proj_land,
    reduced,
    readout_v,
    mixed_send,
    mixed_land,
    mixed_all,
    mix_send,
    mix_land,
    after_v,
    load_sem,
    store_sem,
    all_send,
    all_recv,
    tp_send,
    tp_recv,
    kv_send,
    kv_recv,
):
    total = kv_count * tp_count
    my_kv = lax.axis_index("kv")
    my_tp = lax.axis_index("tp")
    me = my_kv * tp_count + my_tp
    rows, chunk = tokens.shape
    block = tp_count * chunk
    model_width = total * chunk
    seq_local, heads_local, key_width, value_width = memory.shape

    loads = [
        pltpu.make_async_copy(source, target, load_sem.at[n])
        for n, (source, target) in enumerate(
            (
                (first_gate, gate_a),
                (first_up, up_a),
                (first_down, down_a),
                (query_weight, query_w),
                (key_weight, key_w),
                (value_weight, value_w),
                (outgate_weight, outgate_w),
                (ingate_weight, ingate_w),
                (forget_weight, forget_w),
                (memory, memory_v),
                (mixout_weight, mixout_w),
                (second_gate, gate_b),
                (second_up, up_b),
                (second_down, down_b),
            )
        )
    ]
    for load in loads[:3]:
        load.start()

    barrier = pltpu.get_barrier_semaphore()

    def greet(step, carry):
        peer = (me + step) % total
        pl.semaphore_signal(
            barrier,
            inc=1,
            device_id={"kv": peer // tp_count, "tp": peer % tp_count},
            device_id_type=pl.DeviceIdType.MESH,
        )
        return carry

    lax.fori_loop(1, total, greet, 0)
    pl.semaphore_wait(barrier, total - 1)

    def send(source, target, send_sem, recv_sem, kv_index, tp_index):
        return pltpu.make_async_remote_copy(
            src_ref=source,
            dst_ref=target,
            send_sem=send_sem,
            recv_sem=recv_sem,
            device_id={"kv": kv_index, "tp": tp_index},
            device_id_type=pl.DeviceIdType.MESH,
        )

    def share_all(source, target, phase):
        def step_of(step, carry):
            peer = (me + step) % total
            send(
                source,
                target.at[me],
                all_send.at[phase, peer],
                all_recv.at[phase, me],
                peer // tp_count,
                peer % tp_count,
            ).start()
            return carry

        lax.fori_loop(1, total, step_of, 0)

    def sent_all(source_of, target, phase):
        def step_of(step, carry):
            peer = (me + step) % total
            send(
                source_of(peer),
                target.at[me],
                all_send.at[phase, peer],
                all_recv.at[phase, me],
                peer // tp_count,
                peer % tp_count,
            ).wait_send()
            return carry

        lax.fori_loop(1, total, step_of, 0)

    def arrived(target, phase, peer):
        send(
            target.at[peer],
            target.at[peer],
            all_send.at[phase, peer],
            all_recv.at[phase, peer],
            peer // tp_count,
            peer % tp_count,
        ).wait_recv()

    def half(own, gain, gate_w, up_w, down_w, gathered, parts, landed, phase, ready):
        share_all(own, gathered, phase)
        gathered[me] = own[...]
        ready(0)
        hidden_units = gate_w.shape[1]

        def group_of(step, carry):
            gate_sum, up_sum, squares = carry
            group = (my_kv + step) % kv_count
            for t in range(tp_count):
                peer = group * tp_count + t

                @pl.when(peer != me)
                def _():
                    arrived(gathered, phase, peer)

            wide = jnp.concatenate(
                [gathered[group * tp_count + t].astype(jnp.float32) for t in range(tp_count)],
                axis=1,
            )
            start = pl.multiple_of(group * block, block)
            normed = (wide * gain[:, pl.ds(start, block)].astype(jnp.float32)).astype(jnp.bfloat16)
            gate_sum = gate_sum + jnp.dot(
                normed, gate_w[pl.ds(start, block), :], preferred_element_type=jnp.float32
            )
            up_sum = up_sum + jnp.dot(
                normed, up_w[pl.ds(start, block), :], preferred_element_type=jnp.float32
            )
            return gate_sum, up_sum, squares + jnp.sum(wide * wide, axis=1, keepdims=True)

        zero = jnp.zeros((rows, hidden_units), jnp.float32)
        gate_sum, up_sum, squares = lax.fori_loop(
            0, kv_count, group_of, (zero, zero, jnp.zeros((rows, 1), jnp.float32))
        )
        factor = lax.rsqrt(squares / model_width + epsilon)
        gate_sum = factor * gate_sum
        hidden = (gate_sum / (1.0 + jnp.exp(-gate_sum)) * (factor * up_sum)).astype(jnp.bfloat16)
        ready(1)

        def ship(group):
            for t in range(tp_count):
                peer = group * tp_count + t

                @pl.when(peer != me)
                def _():
                    send(
                        parts.at[peer],
                        landed.at[me],
                        all_send.at[phase + 1, peer],
                        all_recv.at[phase + 1, me],
                        group,
                        t,
                    ).start()

        def down_of(step, carry):
            group = (my_kv + 1 + step) % kv_count
            start = pl.multiple_of(group * block, block)
            part = jnp.dot(
                hidden, down_w[:, pl.ds(start, block)], preferred_element_type=jnp.float32
            ).astype(jnp.bfloat16)
            for t in range(tp_count):
                parts[group * tp_count + t] = part[:, t * chunk : (t + 1) * chunk]

            @pl.when(step > 0)
            def _():
                ship((my_kv + step) % kv_count)

            return carry

        lax.fori_loop(0, kv_count, down_of, 0)
        ship(my_kv)

        def add_of(step, carry):
            peer = (me + step) % total
            arrived(landed, phase + 1, peer)
            return carry + landed[peer].astype(jnp.float32)

        branch = lax.fori_loop(1, total, add_of, parts[me].astype(jnp.float32))
        return (own[...].astype(jnp.float32) + 0.5 * branch).astype(jnp.bfloat16)

    def ready_a(stage):
        if stage == 0:
            for load in loads[3:]:
                load.start()
            loads[0].wait()
            loads[1].wait()
            proj_send[...] = jnp.zeros_like(proj_send)
            reduced[...] = jnp.zeros_like(reduced)
            readout_v[...] = jnp.zeros_like(readout_v)
        else:
            loads[2].wait()

    def ready_b(stage):
        if stage == 0:
            loads[11].wait()
            loads[12].wait()
        else:
            loads[13].wait()

    first = half(
        tokens, first_gain, gate_a, up_a, down_a, gathered_a, parts_a, landed_a, 0, ready_a
    )
    first_v[...] = first

    def tp_copy(source, target, phase, index):
        return send(
            source, target.at[my_tp], tp_send.at[phase, index], tp_recv.at[phase, my_tp], my_kv, index
        )

    def tp_arrived(target, phase, index):
        send(
            target.at[index],
            target.at[index],
            tp_send.at[phase, index],
            tp_recv.at[phase, index],
            my_kv,
            index,
        ).wait_recv()

    def kv_copy(source, target, phase, index):
        return send(
            source, target.at[my_kv], kv_send.at[phase, index], kv_recv.at[phase, my_kv], index, my_tp
        )

    def kv_arrived(target, phase, index):
        send(
            target.at[index],
            target.at[index],
            kv_send.at[phase, index],
            kv_recv.at[phase, index],
            index,
            my_tp,
        ).wait_recv()

    for step in range(1, tp_count):
        tp_copy(first_v, block_v, 0, (my_tp + step) % tp_count).start()
    block_v[my_tp] = first
    for load in loads[3:9]:
        load.wait()
    for step in range(1, tp_count):
        tp_arrived(block_v, 0, (my_tp + step) % tp_count)
    wide = jnp.concatenate([block_v[t].astype(jnp.float32) for t in range(tp_count)], axis=1)
    start = pl.multiple_of(my_kv * block, block)
    normed = (wide * mix_gain[:, pl.ds(start, block)].astype(jnp.float32)).astype(jnp.bfloat16)
    offsets = [0]
    for weight in (query_w, key_w, value_w, outgate_w):
        offsets.append(offsets[-1] + weight.shape[1])
    edge = offsets[-1]
    lane = 128
    head_count = ingate_w.shape[1]
    pieces = [
        (offset, jnp.dot(normed, weight[...], preferred_element_type=jnp.float32))
        for offset, weight in zip(
            offsets[:4] + [edge, edge + lane],
            (query_w, key_w, value_w, outgate_w, ingate_w, forget_w),
        )
    ]
    squares = jnp.broadcast_to(jnp.sum(wide * wide, axis=1, keepdims=True), (rows, lane))
    pieces.append((edge + 2 * lane, squares))
    for k in range(kv_count):
        for offset, piece in pieces:
            proj_send[k, :, offset : offset + piece.shape[1]] = piece[
                k * seq_local : (k + 1) * seq_local, :
            ]
    for step in range(1, kv_count):
        peer = (my_kv + step) % kv_count
        kv_copy(proj_send.at[peer], proj_land, 0, peer).start()
    loads[9].wait()
    summed = proj_send[my_kv]
    for step in range(1, kv_count):
        peer = (my_kv + step) % kv_count
        kv_arrived(proj_land, 0, peer)
        summed = summed + proj_land[peer]
    reduced[0:seq_local, :] = summed
    everything = reduced[...]
    factor = lax.rsqrt(everything[:, edge + 2 * lane : edge + 2 * lane + 1] / model_width + epsilon)
    query, keys, values, outgate = [
        (factor * everything[:, offsets[n] : offsets[n + 1]]).astype(jnp.bfloat16).astype(jnp.float32)
        for n in range(4)
    ]
    ingate_sum = everything[:, edge : edge + head_count]
    forget_sum = everything[:, edge + lane : edge + lane + head_count]
    ingate = ingate_sum[:, 0:heads_local]
    forget = forget_sum[:, 0:heads_local]
    for t in range(1, tp_count):
        here = my_tp == t
        ingate = jnp.where(here, ingate_sum[:, t * heads_local : (t + 1) * heads_local], ingate)
        forget = jnp.where(here, forget_sum[:, t * heads_local : (t + 1) * heads_local], forget)
    ingate = (factor * ingate)[0:seq_local]
    forget = (factor * forget)[0:seq_local] + forget_bias[...]
    log_forget = jnp.minimum(forget, 0.0) - jnp.log1p(jnp.exp(-jnp.abs(forget)))
    shifted = log_forget + stabilizer[...]
    ceiling = jnp.maximum(shifted, ingate)
    retain = jnp.exp(shifted - ceiling)
    admission = jnp.exp(ingate - ceiling) * key_width ** (-0.5)
    ceiling_out[...] = ceiling
    row_index = lax.broadcasted_iota(jnp.int32, (reduced.shape[0], key_width), 0)
    stores = []
    for h in range(heads_local):
        head_keys = keys[:, h * key_width : (h + 1) * key_width]
        head_values = values[:, h * value_width : (h + 1) * value_width]
        head_query = query[:, h * key_width : (h + 1) * key_width]
        for s in range(seq_local):
            outer = lax.dot_general(
                jnp.where(row_index == s, head_keys, 0.0),
                head_values,
                (((0,), (0,)), ((), ())),
                preferred_element_type=jnp.float32,
            )
            updated = (
                retain[s : s + 1, h : h + 1] * memory_v[s, h]
                + admission[s : s + 1, h : h + 1] * outer
            )
            memory_v[s, h] = updated
            read = jnp.dot(
                head_query,
                updated,
                precision=lax.Precision.HIGHEST,
                preferred_element_type=jnp.float32,
            )
            readout_v[s : s + 1, h * value_width : (h + 1) * value_width] = read[s : s + 1, :]
    store = pltpu.make_async_copy(memory_v, memory_next, store_sem)
    for h in range(heads_local):
        span = slice(h * value_width, (h + 1) * value_width)
        readout = readout_v[:, span]
        normalized = readout * lax.rsqrt(
            jnp.mean(readout * readout, axis=-1, keepdims=True) + epsilon
        )
        gated = (
            normalized * head_gain[:, span].astype(jnp.float32) / (1.0 + jnp.exp(-outgate[:, span]))
        )
        mixed_send[:, span] = gated.astype(jnp.bfloat16).astype(jnp.float32)[0:seq_local, :]
    store.start()
    for step in range(1, kv_count):
        kv_copy(mixed_send, mixed_land, 1, (my_kv + step) % kv_count).start()
    mixed_land[my_kv] = mixed_send[...]
    loads[10].wait()
    for step in range(1, kv_count):
        kv_arrived(mixed_land, 1, (my_kv + step) % kv_count)
    for k in range(kv_count):
        mixed_all[k * seq_local : (k + 1) * seq_local, :] = mixed_land[k]
    mix_terms = jnp.dot(
        mixed_all[...].astype(jnp.bfloat16), mixout_w[...], preferred_element_type=jnp.float32
    ).astype(jnp.bfloat16)
    for t in range(tp_count):
        mix_send[t] = mix_terms[:, t * chunk : (t + 1) * chunk]
    for step in range(1, tp_count):
        peer = (my_tp + step) % tp_count
        tp_copy(mix_send.at[peer], mix_land, 1, peer).start()
    branch = mix_send[my_tp].astype(jnp.float32)
    for step in range(1, tp_count):
        peer = (my_tp + step) % tp_count
        tp_arrived(mix_land, 1, peer)
        branch = branch + mix_land[peer].astype(jnp.float32)
    after_v[...] = (first.astype(jnp.float32) + branch).astype(jnp.bfloat16)
    layer_out[...] = half(
        after_v, second_gain, gate_b, up_b, down_b, gathered_b, parts_b, landed_b, 2, ready_b
    )

    sent_all(lambda peer: tokens, gathered_a, 0)
    sent_all(lambda peer: parts_a.at[peer], landed_a, 1)
    sent_all(lambda peer: after_v, gathered_b, 2)
    sent_all(lambda peer: parts_b.at[peer], landed_b, 3)
    for step in range(1, tp_count):
        peer = (my_tp + step) % tp_count
        tp_copy(first_v, block_v, 0, peer).wait_send()
        tp_copy(mix_send.at[peer], mix_land, 1, peer).wait_send()
    for step in range(1, kv_count):
        peer = (my_kv + step) % kv_count
        kv_copy(proj_send.at[peer], proj_land, 0, peer).wait_send()
        kv_copy(mixed_send, mixed_land, 1, peer).wait_send()
    store.wait()


def fused_on_device(
    kv_count,
    tp_count,
    tokens,
    first_gain,
    first_gate,
    first_up,
    first_down,
    mix_gain,
    query_weight,
    key_weight,
    value_weight,
    outgate_weight,
    ingate_weight,
    forget_weight,
    forget_bias,
    head_gain,
    mixout_weight,
    memory,
    stabilizer,
    second_gain,
    second_gate,
    second_up,
    second_down,
):
    total = kv_count * tp_count
    rows, chunk = tokens.shape
    seq_local = memory.shape[0]
    width = sum(w.shape[1] for w in (query_weight, key_weight, value_weight, outgate_weight)) + 384
    mixed_width = outgate_weight.shape[1]
    held_rows = max(8, seq_local)

    def like(array):
        return pltpu.VMEM(array.shape, array.dtype)

    exchange = pltpu.VMEM((total, rows, chunk), jnp.bfloat16)
    tile = pltpu.VMEM((rows, chunk), jnp.bfloat16)
    tp_tiles = pltpu.VMEM((tp_count, rows, chunk), jnp.bfloat16)
    vmem = pl.BlockSpec(memory_space=pltpu.VMEM)
    hbm = pl.BlockSpec(memory_space=pl.ANY)
    return pl.pallas_call(
        functools.partial(fused_kernel, kv_count, tp_count),
        out_shape=(
            jax.ShapeDtypeStruct(tokens.shape, jnp.bfloat16),
            jax.ShapeDtypeStruct(memory.shape, memory.dtype),
            jax.ShapeDtypeStruct(stabilizer.shape, stabilizer.dtype),
        ),
        in_specs=[vmem] * 7 + [hbm] * 14,
        out_specs=(vmem, hbm, vmem),
        scratch_shapes=[
            like(first_gate),
            like(first_up),
            like(first_down),
            like(second_gate),
            like(second_up),
            like(second_down),
            like(query_weight),
            like(key_weight),
            like(value_weight),
            like(outgate_weight),
            like(ingate_weight),
            like(forget_weight),
            like(mixout_weight),
            like(memory),
            exchange,
            exchange,
            exchange,
            exchange,
            exchange,
            exchange,
            tile,
            tp_tiles,
            pltpu.VMEM((kv_count, seq_local, width), jnp.float32),
            pltpu.VMEM((kv_count, seq_local, width), jnp.float32),
            pltpu.VMEM((held_rows, width), jnp.float32),
            pltpu.VMEM((held_rows, mixed_width), jnp.float32),
            pltpu.VMEM((seq_local, mixed_width), jnp.float32),
            pltpu.VMEM((kv_count, seq_local, mixed_width), jnp.float32),
            pltpu.VMEM((rows, mixed_width), jnp.float32),
            tp_tiles,
            tp_tiles,
            tile,
            pltpu.SemaphoreType.DMA((14,)),
            pltpu.SemaphoreType.DMA,
            pltpu.SemaphoreType.DMA((4, total)),
            pltpu.SemaphoreType.DMA((4, total)),
            pltpu.SemaphoreType.DMA((2, tp_count)),
            pltpu.SemaphoreType.DMA((2, tp_count)),
            pltpu.SemaphoreType.DMA((2, kv_count)),
            pltpu.SemaphoreType.DMA((2, kv_count)),
        ],
        compiler_params=pltpu.CompilerParams(
            collective_id=0, has_side_effects=True, vmem_limit_bytes=60 * 1024 * 1024
        ),
    )(
        tokens,
        first_gain[None, :],
        mix_gain[None, :],
        second_gain[None, :],
        head_gain[None, :],
        forget_bias[None, :],
        stabilizer,
        first_gate,
        first_up,
        first_down,
        query_weight,
        key_weight,
        value_weight,
        outgate_weight,
        ingate_weight,
        forget_weight,
        mixout_weight,
        memory,
        second_gate,
        second_up,
        second_down,
    )


def choose(kv_count, tp_count, *arrays):
    if arrays[0].shape[1] % 128 == 0:
        return fused_on_device(kv_count, tp_count, *arrays)
    return on_device(*arrays)


def solution(mesh):
    in_specs = (
        P(None, ("kv", "tp")),
        P(),
        P(None, ("kv", "tp")),
        P(None, ("kv", "tp")),
        P(("kv", "tp"), None),
        P(),
        P("kv", "tp"),
        P("kv", "tp"),
        P("kv", "tp"),
        P("kv", "tp"),
        P("kv", None),
        P("kv", None),
        P("tp"),
        P("tp"),
        P("tp", "kv"),
        P("kv", "tp", None, None),
        P("kv", "tp"),
        P(),
        P(None, ("kv", "tp")),
        P(None, ("kv", "tp")),
        P(("kv", "tp"), None),
    )
    out_specs = (P(None, ("kv", "tp")), P("kv", "tp", None, None), P("kv", "tp"))
    return jax.shard_map(
        functools.partial(choose, mesh.shape["kv"], mesh.shape["tp"]),
        mesh=mesh,
        in_specs=in_specs, out_specs=out_specs, check_vma=False
    )
```

```python
import functools

import jax
import jax.numpy as jnp
from jax import lax
from jax.experimental import pallas as pl
from jax.experimental.pallas import tpu as pltpu
from jax.sharding import PartitionSpec as P

epsilon = 1e-06


def row_scale(squares, model_width):
    return lax.rsqrt(squares / model_width + epsilon)[:, None]


def fold_columns(column_block, gain_vector, matrices):
    wide_block = column_block.astype(jnp.float32)
    gain_piece = gain_vector.astype(jnp.float32)
    normed = (wide_block * gain_piece).astype(jnp.bfloat16)
    updated = tuple(
        (jnp.dot(normed, matrix, preferred_element_type=jnp.float32) for matrix in matrices)
    )
    return (updated, jnp.sum(wide_block * wide_block, axis=1))


def half_mlp(tokens, norm_gain, gate_weight, up_weight, down_weight):
    model_width = norm_gain.shape[0]
    (gate_sum, up_sum), squares = fold_columns(
        lax.all_gather(tokens, ("kv", "tp"), axis=1, tiled=True),
        norm_gain,
        (gate_weight, up_weight),
    )
    row_factor = row_scale(squares, model_width)
    hidden = (jax.nn.silu(row_factor * gate_sum) * (row_factor * up_sum)).astype(jnp.bfloat16)
    branch = lax.psum_scatter(
        lax.dot_general(
            down_weight, hidden, (((0,), (1,)), ((), ())), preferred_element_type=jnp.float32
        ),
        ("kv", "tp"),
        scatter_dimension=0,
        tiled=True,
    ).T
    return (tokens.astype(jnp.float32) + 0.5 * branch).astype(jnp.bfloat16)


def on_device(
    tokens,
    first_gain,
    first_gate,
    first_up,
    first_down,
    mix_gain,
    query_weight,
    key_weight,
    value_weight,
    outgate_weight,
    ingate_weight,
    forget_weight,
    forget_bias,
    head_gain,
    mixout_weight,
    memory,
    stabilizer,
    second_gain,
    second_gate,
    second_up,
    second_down,
):
    first = half_mlp(tokens, first_gain, first_gate, first_up, first_down)
    matrices = (
        query_weight,
        key_weight,
        value_weight,
        outgate_weight,
        ingate_weight,
        forget_weight,
    )
    block_width = query_weight.shape[0]
    gain_block = lax.dynamic_slice_in_dim(
        mix_gain, lax.axis_index("kv") * block_width, block_width, 0
    )
    mix_partials, squares = fold_columns(
        lax.all_gather(first, "tp", axis=1, tiled=True), gain_block, matrices
    )
    query_sum, key_sum, value_sum, outgate_sum, ingate_sum, forget_sum, squares = (
        lax.psum_scatter(mix_partials[0], "kv", scatter_dimension=0, tiled=True),
        lax.psum_scatter(mix_partials[1], "kv", scatter_dimension=0, tiled=True),
        lax.psum_scatter(mix_partials[2], "kv", scatter_dimension=0, tiled=True),
        lax.psum_scatter(mix_partials[3], "kv", scatter_dimension=0, tiled=True),
        lax.psum_scatter(mix_partials[4], "kv", scatter_dimension=0, tiled=True),
        lax.psum_scatter(mix_partials[5], "kv", scatter_dimension=0, tiled=True),
        lax.psum_scatter(squares, "kv", scatter_dimension=0, tiled=True),
    )
    row_factor = row_scale(squares, mix_gain.shape[0])
    seq_local, heads_local, key_width, value_width = memory.shape
    query = (row_factor * query_sum).astype(jnp.bfloat16).reshape(seq_local, heads_local, key_width)
    keys = (row_factor * key_sum).astype(jnp.bfloat16).reshape(seq_local, heads_local, key_width)
    values = (
        (row_factor * value_sum).astype(jnp.bfloat16).reshape(seq_local, heads_local, value_width)
    )
    outgate = (
        (row_factor * outgate_sum).astype(jnp.bfloat16).reshape(seq_local, heads_local, value_width)
    )
    head_start = lax.axis_index("tp") * heads_local
    ingate = lax.dynamic_slice_in_dim(row_factor * ingate_sum, head_start, heads_local, 1)
    forget = (
        lax.dynamic_slice_in_dim(row_factor * forget_sum, head_start, heads_local, 1)
        + forget_bias[None, :]
    )
    log_forget = jax.nn.log_sigmoid(forget)
    ceiling = jnp.maximum(log_forget + stabilizer, ingate)
    retain = jnp.exp(log_forget + stabilizer - ceiling)
    admission = jnp.exp(ingate - ceiling)
    scaled_keys = keys.astype(jnp.float32) * key_width ** (-0.5)
    outer_product = jnp.einsum("shd,she->shde", scaled_keys, values.astype(jnp.float32))
    memory_next = retain[..., None, None] * memory + admission[..., None, None] * outer_product
    readout = jnp.einsum(
        "shd,shde->she", query.astype(jnp.float32), memory_next, precision=lax.Precision.HIGHEST
    )
    normalized = readout * lax.rsqrt(jnp.mean(readout * readout, axis=-1, keepdims=True) + epsilon)
    gated = (
        normalized
        * head_gain.reshape(heads_local, value_width).astype(jnp.float32)
        * jax.nn.sigmoid(outgate.astype(jnp.float32))
    )
    mixed = gated.reshape(seq_local, heads_local * value_width).astype(jnp.bfloat16)
    mix_terms = jnp.dot(
        lax.all_gather(mixed, "kv", axis=0, tiled=True),
        mixout_weight,
        preferred_element_type=jnp.float32,
    )
    mix_branch = lax.psum_scatter(
        mix_terms.astype(jnp.bfloat16), "tp", scatter_dimension=1, tiled=True
    ).astype(jnp.float32)
    after_mix = (first.astype(jnp.float32) + mix_branch).astype(jnp.bfloat16)
    layer_out = half_mlp(after_mix, second_gain, second_gate, second_up, second_down)
    return (layer_out, memory_next, ceiling)


def fused_kernel(
    kv_count,
    tp_count,
    tokens,
    first_gain,
    mix_gain,
    second_gain,
    head_gain,
    forget_bias,
    stabilizer,
    first_gate,
    first_up,
    first_down,
    query_weight,
    key_weight,
    value_weight,
    outgate_weight,
    ingate_weight,
    forget_weight,
    mixout_weight,
    memory,
    second_gate,
    second_up,
    second_down,
    layer_out,
    memory_next,
    ceiling_out,
    gate_a,
    up_a,
    down_a,
    gate_b,
    up_b,
    down_b,
    query_w,
    key_w,
    value_w,
    outgate_w,
    ingate_w,
    forget_w,
    mixout_w,
    memory_v,
    gathered_a,
    parts_a,
    landed_a,
    gathered_b,
    parts_b,
    landed_b,
    first_v,
    block_v,
    proj_send,
    proj_land,
    reduced,
    readout_v,
    mixed_send,
    mixed_land,
    mixed_all,
    mix_send,
    mix_land,
    after_v,
    load_sem,
    store_sem,
    all_send,
    all_recv,
    tp_send,
    tp_recv,
    kv_send,
    kv_recv,
):
    total = kv_count * tp_count
    wide_dims = (((1,), (1,)), ((), ()))
    my_kv = lax.axis_index("kv")
    my_tp = lax.axis_index("tp")
    me = my_kv * tp_count + my_tp
    rows, chunk = tokens.shape
    block = tp_count * chunk
    model_width = total * chunk
    seq_local, heads_local, key_width, value_width = memory.shape

    loads = [
        pltpu.make_async_copy(source, target, load_sem.at[n])
        for n, (source, target) in enumerate(
            (
                (first_gate, gate_a),
                (first_up, up_a),
                (first_down, down_a),
                (query_weight, query_w),
                (key_weight, key_w),
                (value_weight, value_w),
                (outgate_weight, outgate_w),
                (ingate_weight, ingate_w),
                (forget_weight, forget_w),
                (memory, memory_v),
                (mixout_weight, mixout_w),
                (second_gate, gate_b),
                (second_up, up_b),
                (second_down, down_b),
            )
        )
    ]
    for load in loads[:3]:
        load.start()

    barrier = pltpu.get_barrier_semaphore()

    def greet(step, carry):
        peer = (me + step) % total
        pl.semaphore_signal(
            barrier,
            inc=1,
            device_id={"kv": peer // tp_count, "tp": peer % tp_count},
            device_id_type=pl.DeviceIdType.MESH,
        )
        return carry

    lax.fori_loop(1, total, greet, 0)
    pl.semaphore_wait(barrier, total - 1)

    def send(source, target, send_sem, recv_sem, kv_index, tp_index):
        return pltpu.make_async_remote_copy(
            src_ref=source,
            dst_ref=target,
            send_sem=send_sem,
            recv_sem=recv_sem,
            device_id={"kv": kv_index, "tp": tp_index},
            device_id_type=pl.DeviceIdType.MESH,
        )

    partner_tp = my_tp + 1 - 2 * (my_tp % 2)

    def twin(peer):
        return peer + 1 - 2 * (peer % 2)

    def direct(source, target, phase, peer):
        return send(
            source,
            target.at[me],
            all_send.at[phase, peer],
            all_recv.at[phase, me],
            peer // tp_count,
            peer % tp_count,
        )

    def forward(source, target, phase, peer):
        return send(
            source,
            target.at[peer],
            all_send.at[phase, twin(peer)],
            all_recv.at[phase, peer],
            my_kv,
            partner_tp,
        )

    def share_all(source, target, phase):
        def step_of(step, carry):
            direct(source, target, phase, (me + 2 * step) % total).start()
            return carry

        forward(source, target, phase, me).start()
        lax.fori_loop(1, total // 2, step_of, 0)

    def shared_all(source, target, phase):
        def step_of(step, carry):
            peer = (me + 2 * step) % total
            direct(source, target, phase, peer).wait_send()
            forward(target.at[peer], target, phase, peer).wait_send()
            return carry

        forward(source, target, phase, me).wait_send()
        lax.fori_loop(1, total // 2, step_of, 0)

    def sent_all(source, target, phase):
        def step_of(step, carry):
            peer = (me + step) % total
            direct(source.at[peer], target, phase, peer).wait_send()
            return carry

        lax.fori_loop(1, total, step_of, 0)

    def arrived(target, phase, peer):
        send(
            target.at[peer],
            target.at[peer],
            all_send.at[phase, peer],
            all_recv.at[phase, peer],
            peer // tp_count,
            peer % tp_count,
        ).wait_recv()

    def half(own, gain, gate_w, up_w, down_w, gathered, parts, landed, phase, ready):
        share_all(own, gathered, phase)
        gathered[me] = own[...]
        ready(0)
        hidden_units = gate_w.shape[0]

        def group_of(step, carry):
            gate_sum, up_sum, squares = carry
            group = (my_kv + step) % kv_count

            @pl.when(step < kv_count - 1)
            def _():
                relay((my_kv + step + 1) % kv_count)

            for pair in range(tp_count // 2):
                arrived(gathered, phase, group * tp_count + 2 * pair + 1 - my_tp % 2)

            wide = jnp.concatenate(
                [gathered[group * tp_count + t].astype(jnp.float32) for t in range(tp_count)],
                axis=1,
            )
            start = pl.multiple_of(group * block, block)
            normed = (wide * gain[:, pl.ds(start, block)].astype(jnp.float32)).astype(jnp.bfloat16)
            gate_sum = gate_sum + lax.dot_general(
                normed, gate_w[:, pl.ds(start, block)], wide_dims, preferred_element_type=jnp.float32
            )
            up_sum = up_sum + lax.dot_general(
                normed, up_w[:, pl.ds(start, block)], wide_dims, preferred_element_type=jnp.float32
            )
            return gate_sum, up_sum, squares + jnp.sum(wide * wide, axis=1, keepdims=True)

        def relay(group):
            for pair in range(tp_count // 2):
                peer = group * tp_count + 2 * pair + my_tp % 2

                @pl.when(peer != me)
                def _():
                    arrived(gathered, phase, peer)
                    forward(gathered.at[peer], gathered, phase, peer).start()

        relay(my_kv)
        zero = jnp.zeros((rows, hidden_units), jnp.float32)
        gate_sum, up_sum, squares = lax.fori_loop(
            0, kv_count, group_of, (zero, zero, jnp.zeros((rows, 1), jnp.float32))
        )
        factor = lax.rsqrt(squares / model_width + epsilon)
        gate_sum = factor * gate_sum
        hidden = (gate_sum / (1.0 + jnp.exp(-gate_sum)) * (factor * up_sum)).astype(jnp.bfloat16)
        ready(1)

        def ship(group):
            for t in range(tp_count):
                peer = group * tp_count + t

                @pl.when(peer != me)
                def _():
                    direct(parts.at[peer], landed, phase + 1, peer).start()

        def down_of(step, carry):
            group = (my_kv + 1 + step) % kv_count
            start = pl.multiple_of(group * block, block)
            part = jnp.dot(
                hidden, down_w[:, pl.ds(start, block)], preferred_element_type=jnp.float32
            ).astype(jnp.bfloat16)
            for t in range(tp_count):
                parts[group * tp_count + t] = part[:, t * chunk : (t + 1) * chunk]

            @pl.when(step > 0)
            def _():
                ship((my_kv + step) % kv_count)

            return carry

        lax.fori_loop(0, kv_count, down_of, 0)
        ship(my_kv)

        def add_of(step, carry):
            peer = (me + step) % total
            arrived(landed, phase + 1, peer)
            return carry + landed[peer].astype(jnp.float32)

        branch = lax.fori_loop(1, total, add_of, parts[me].astype(jnp.float32))
        return (own[...].astype(jnp.float32) + 0.5 * branch).astype(jnp.bfloat16)

    def ready_a(stage):
        if stage == 0:
            for load in loads[3:]:
                load.start()
            loads[0].wait()
            loads[1].wait()
            proj_send[...] = jnp.zeros_like(proj_send)
            reduced[...] = jnp.zeros_like(reduced)
            readout_v[...] = jnp.zeros_like(readout_v)
        else:
            loads[2].wait()

    def ready_b(stage):
        if stage == 0:
            loads[11].wait()
            loads[12].wait()
        else:
            loads[13].wait()

    first = half(
        tokens, first_gain, gate_a, up_a, down_a, gathered_a, parts_a, landed_a, 0, ready_a
    )
    first_v[...] = first

    def tp_copy(source, target, phase, index):
        return send(
            source, target.at[my_tp], tp_send.at[phase, index], tp_recv.at[phase, my_tp], my_kv, index
        )

    def tp_arrived(target, phase, index):
        send(
            target.at[index],
            target.at[index],
            tp_send.at[phase, index],
            tp_recv.at[phase, index],
            my_kv,
            index,
        ).wait_recv()

    def kv_copy(source, target, phase, index):
        return send(
            source, target.at[my_kv], kv_send.at[phase, index], kv_recv.at[phase, my_kv], index, my_tp
        )

    def kv_arrived(target, phase, index):
        send(
            target.at[index],
            target.at[index],
            kv_send.at[phase, index],
            kv_recv.at[phase, index],
            index,
            my_tp,
        ).wait_recv()

    for step in range(1, tp_count):
        tp_copy(first_v, block_v, 0, (my_tp + step) % tp_count).start()
    block_v[my_tp] = first
    for load in loads[3:9]:
        load.wait()
    for step in range(1, tp_count):
        tp_arrived(block_v, 0, (my_tp + step) % tp_count)
    wide = jnp.concatenate([block_v[t].astype(jnp.float32) for t in range(tp_count)], axis=1)
    start = pl.multiple_of(my_kv * block, block)
    normed = (wide * mix_gain[:, pl.ds(start, block)].astype(jnp.float32)).astype(jnp.bfloat16)
    offsets = [0]
    for weight in (query_w, key_w, value_w, outgate_w):
        offsets.append(offsets[-1] + weight.shape[1])
    edge = offsets[-1]
    lane = 128
    head_count = ingate_w.shape[0]
    pieces = [
        (offset, jnp.dot(normed, weight[...], preferred_element_type=jnp.float32))
        for offset, weight in zip(
            offsets, (query_w, key_w, value_w, outgate_w)
        )
    ] + [
        (
            edge + n * lane,
            lax.dot_general(normed, weight[...], wide_dims, preferred_element_type=jnp.float32),
        )
        for n, weight in enumerate((ingate_w, forget_w))
    ]
    squares = jnp.broadcast_to(jnp.sum(wide * wide, axis=1, keepdims=True), (rows, lane))
    pieces.append((edge + 2 * lane, squares))
    for k in range(kv_count):
        for offset, piece in pieces:
            proj_send[k, :, offset : offset + piece.shape[1]] = piece[
                k * seq_local : (k + 1) * seq_local, :
            ]
    for step in range(1, kv_count):
        peer = (my_kv + step) % kv_count
        kv_copy(proj_send.at[peer], proj_land, 0, peer).start()
    loads[9].wait()
    summed = proj_send[my_kv]
    for step in range(1, kv_count):
        peer = (my_kv + step) % kv_count
        kv_arrived(proj_land, 0, peer)
        summed = summed + proj_land[peer]
    reduced[0:seq_local, :] = summed
    everything = reduced[...]
    factor = lax.rsqrt(everything[:, edge + 2 * lane : edge + 2 * lane + 1] / model_width + epsilon)
    query, keys, values, outgate = [
        (factor * everything[:, offsets[n] : offsets[n + 1]]).astype(jnp.bfloat16).astype(jnp.float32)
        for n in range(4)
    ]
    ingate_sum = everything[:, edge : edge + head_count]
    forget_sum = everything[:, edge + lane : edge + lane + head_count]
    ingate = ingate_sum[:, 0:heads_local]
    forget = forget_sum[:, 0:heads_local]
    for t in range(1, tp_count):
        here = my_tp == t
        ingate = jnp.where(here, ingate_sum[:, t * heads_local : (t + 1) * heads_local], ingate)
        forget = jnp.where(here, forget_sum[:, t * heads_local : (t + 1) * heads_local], forget)
    ingate = (factor * ingate)[0:seq_local]
    forget = (factor * forget)[0:seq_local] + forget_bias[...]
    log_forget = jnp.minimum(forget, 0.0) - jnp.log1p(jnp.exp(-jnp.abs(forget)))
    shifted = log_forget + stabilizer[...]
    ceiling = jnp.maximum(shifted, ingate)
    retain = jnp.exp(shifted - ceiling)
    admission = jnp.exp(ingate - ceiling) * key_width ** (-0.5)
    ceiling_out[...] = ceiling
    row_index = lax.broadcasted_iota(jnp.int32, (reduced.shape[0], key_width), 0)
    stores = []
    for h in range(heads_local):
        head_keys = keys[:, h * key_width : (h + 1) * key_width]
        head_values = values[:, h * value_width : (h + 1) * value_width]
        head_query = query[:, h * key_width : (h + 1) * key_width]
        for s in range(seq_local):
            outer = lax.dot_general(
                jnp.where(row_index == s, head_keys, 0.0),
                head_values,
                (((0,), (0,)), ((), ())),
                preferred_element_type=jnp.float32,
            )
            updated = (
                retain[s : s + 1, h : h + 1] * memory_v[s, h]
                + admission[s : s + 1, h : h + 1] * outer
            )
            memory_v[s, h] = updated
            read = jnp.dot(
                head_query,
                updated,
                precision=lax.Precision.HIGHEST,
                preferred_element_type=jnp.float32,
            )
            readout_v[s : s + 1, h * value_width : (h + 1) * value_width] = read[s : s + 1, :]
    store = pltpu.make_async_copy(memory_v, memory_next, store_sem)
    for h in range(heads_local):
        span = slice(h * value_width, (h + 1) * value_width)
        readout = readout_v[:, span]
        normalized = readout * lax.rsqrt(
            jnp.mean(readout * readout, axis=-1, keepdims=True) + epsilon
        )
        gated = (
            normalized * head_gain[:, span].astype(jnp.float32) / (1.0 + jnp.exp(-outgate[:, span]))
        )
        mixed_send[:, span] = gated.astype(jnp.bfloat16).astype(jnp.float32)[0:seq_local, :]
    store.start()
    for step in range(1, kv_count):
        kv_copy(mixed_send, mixed_land, 1, (my_kv + step) % kv_count).start()
    mixed_land[my_kv] = mixed_send[...]
    loads[10].wait()
    for step in range(1, kv_count):
        kv_arrived(mixed_land, 1, (my_kv + step) % kv_count)
    for k in range(kv_count):
        mixed_all[k * seq_local : (k + 1) * seq_local, :] = mixed_land[k]
    mix_terms = jnp.dot(
        mixed_all[...].astype(jnp.bfloat16), mixout_w[...], preferred_element_type=jnp.float32
    ).astype(jnp.bfloat16)
    for t in range(tp_count):
        mix_send[t] = mix_terms[:, t * chunk : (t + 1) * chunk]
    for step in range(1, tp_count):
        peer = (my_tp + step) % tp_count
        tp_copy(mix_send.at[peer], mix_land, 1, peer).start()
    branch = mix_send[my_tp].astype(jnp.float32)
    for step in range(1, tp_count):
        peer = (my_tp + step) % tp_count
        tp_arrived(mix_land, 1, peer)
        branch = branch + mix_land[peer].astype(jnp.float32)
    after_v[...] = (first.astype(jnp.float32) + branch).astype(jnp.bfloat16)
    layer_out[...] = half(
        after_v, second_gain, gate_b, up_b, down_b, gathered_b, parts_b, landed_b, 2, ready_b
    )

    shared_all(tokens, gathered_a, 0)
    sent_all(parts_a, landed_a, 1)
    shared_all(after_v, gathered_b, 2)
    sent_all(parts_b, landed_b, 3)
    for step in range(1, tp_count):
        peer = (my_tp + step) % tp_count
        tp_copy(first_v, block_v, 0, peer).wait_send()
        tp_copy(mix_send.at[peer], mix_land, 1, peer).wait_send()
    for step in range(1, kv_count):
        peer = (my_kv + step) % kv_count
        kv_copy(proj_send.at[peer], proj_land, 0, peer).wait_send()
        kv_copy(mixed_send, mixed_land, 1, peer).wait_send()
    store.wait()


def fused_on_device(
    kv_count,
    tp_count,
    tokens,
    first_gain,
    first_gate,
    first_up,
    first_down,
    mix_gain,
    query_weight,
    key_weight,
    value_weight,
    outgate_weight,
    ingate_weight,
    forget_weight,
    forget_bias,
    head_gain,
    mixout_weight,
    memory,
    stabilizer,
    second_gain,
    second_gate,
    second_up,
    second_down,
):
    total = kv_count * tp_count
    rows, chunk = tokens.shape
    seq_local = memory.shape[0]
    first_gate, first_up, second_gate, second_up = (
        first_gate.T,
        first_up.T,
        second_gate.T,
        second_up.T,
    )
    ingate_weight, forget_weight = ingate_weight.T, forget_weight.T
    width = sum(w.shape[1] for w in (query_weight, key_weight, value_weight, outgate_weight)) + 384
    mixed_width = outgate_weight.shape[1]
    held_rows = max(8, seq_local)

    def like(array):
        return pltpu.VMEM(array.shape, array.dtype)

    exchange = pltpu.VMEM((total, rows, chunk), jnp.bfloat16)
    tile = pltpu.VMEM((rows, chunk), jnp.bfloat16)
    tp_tiles = pltpu.VMEM((tp_count, rows, chunk), jnp.bfloat16)
    vmem = pl.BlockSpec(memory_space=pltpu.VMEM)
    hbm = pl.BlockSpec(memory_space=pl.ANY)
    return pl.pallas_call(
        functools.partial(fused_kernel, kv_count, tp_count),
        out_shape=(
            jax.ShapeDtypeStruct(tokens.shape, jnp.bfloat16),
            jax.ShapeDtypeStruct(memory.shape, memory.dtype),
            jax.ShapeDtypeStruct(stabilizer.shape, stabilizer.dtype),
        ),
        in_specs=[vmem] * 7 + [hbm] * 14,
        out_specs=(vmem, hbm, vmem),
        scratch_shapes=[
            like(first_gate),
            like(first_up),
            like(first_down),
            like(second_gate),
            like(second_up),
            like(second_down),
            like(query_weight),
            like(key_weight),
            like(value_weight),
            like(outgate_weight),
            like(ingate_weight),
            like(forget_weight),
            like(mixout_weight),
            like(memory),
            exchange,
            exchange,
            exchange,
            exchange,
            exchange,
            exchange,
            tile,
            tp_tiles,
            pltpu.VMEM((kv_count, seq_local, width), jnp.float32),
            pltpu.VMEM((kv_count, seq_local, width), jnp.float32),
            pltpu.VMEM((held_rows, width), jnp.float32),
            pltpu.VMEM((held_rows, mixed_width), jnp.float32),
            pltpu.VMEM((seq_local, mixed_width), jnp.float32),
            pltpu.VMEM((kv_count, seq_local, mixed_width), jnp.float32),
            pltpu.VMEM((rows, mixed_width), jnp.float32),
            tp_tiles,
            tp_tiles,
            tile,
            pltpu.SemaphoreType.DMA((14,)),
            pltpu.SemaphoreType.DMA,
            pltpu.SemaphoreType.DMA((4, total)),
            pltpu.SemaphoreType.DMA((4, total)),
            pltpu.SemaphoreType.DMA((2, tp_count)),
            pltpu.SemaphoreType.DMA((2, tp_count)),
            pltpu.SemaphoreType.DMA((2, kv_count)),
            pltpu.SemaphoreType.DMA((2, kv_count)),
        ],
        compiler_params=pltpu.CompilerParams(
            collective_id=0, has_side_effects=True, vmem_limit_bytes=60 * 1024 * 1024
        ),
    )(
        tokens,
        first_gain[None, :],
        mix_gain[None, :],
        second_gain[None, :],
        head_gain[None, :],
        forget_bias[None, :],
        stabilizer,
        first_gate,
        first_up,
        first_down,
        query_weight,
        key_weight,
        value_weight,
        outgate_weight,
        ingate_weight,
        forget_weight,
        mixout_weight,
        memory,
        second_gate,
        second_up,
        second_down,
    )


def choose(kv_count, tp_count, *arrays):
    if arrays[0].shape[1] % 128 == 0 and tp_count % 2 == 0:
        return fused_on_device(kv_count, tp_count, *arrays)
    return on_device(*arrays)


def solution(mesh):
    in_specs = (
        P(None, ("kv", "tp")),
        P(),
        P(None, ("kv", "tp")),
        P(None, ("kv", "tp")),
        P(("kv", "tp"), None),
        P(),
        P("kv", "tp"),
        P("kv", "tp"),
        P("kv", "tp"),
        P("kv", "tp"),
        P("kv", None),
        P("kv", None),
        P("tp"),
        P("tp"),
        P("tp", "kv"),
        P("kv", "tp", None, None),
        P("kv", "tp"),
        P(),
        P(None, ("kv", "tp")),
        P(None, ("kv", "tp")),
        P(("kv", "tp"), None),
    )
    out_specs = (P(None, ("kv", "tp")), P("kv", "tp", None, None), P("kv", "tp"))
    return jax.shard_map(
        functools.partial(choose, mesh.shape["kv"], mesh.shape["tp"]),
        mesh=mesh,
        in_specs=in_specs, out_specs=out_specs, check_vma=False
    )
```

```python
import functools

import jax
import jax.numpy as jnp
from jax import lax
from jax.experimental import pallas as pl
from jax.experimental.pallas import tpu as pltpu
from jax.sharding import PartitionSpec as P

epsilon = 1e-06


def row_scale(squares, model_width):
    return lax.rsqrt(squares / model_width + epsilon)[:, None]


def fold_columns(column_block, gain_vector, matrices):
    wide_block = column_block.astype(jnp.float32)
    gain_piece = gain_vector.astype(jnp.float32)
    normed = (wide_block * gain_piece).astype(jnp.bfloat16)
    updated = tuple(
        (jnp.dot(normed, matrix, preferred_element_type=jnp.float32) for matrix in matrices)
    )
    return (updated, jnp.sum(wide_block * wide_block, axis=1))


def half_mlp(tokens, norm_gain, gate_weight, up_weight, down_weight):
    model_width = norm_gain.shape[0]
    (gate_sum, up_sum), squares = fold_columns(
        lax.all_gather(tokens, ("kv", "tp"), axis=1, tiled=True),
        norm_gain,
        (gate_weight, up_weight),
    )
    row_factor = row_scale(squares, model_width)
    hidden = (jax.nn.silu(row_factor * gate_sum) * (row_factor * up_sum)).astype(jnp.bfloat16)
    branch = lax.psum_scatter(
        lax.dot_general(
            down_weight, hidden, (((0,), (1,)), ((), ())), preferred_element_type=jnp.float32
        ),
        ("kv", "tp"),
        scatter_dimension=0,
        tiled=True,
    ).T
    return (tokens.astype(jnp.float32) + 0.5 * branch).astype(jnp.bfloat16)


def on_device(
    tokens,
    first_gain,
    first_gate,
    first_up,
    first_down,
    mix_gain,
    query_weight,
    key_weight,
    value_weight,
    outgate_weight,
    ingate_weight,
    forget_weight,
    forget_bias,
    head_gain,
    mixout_weight,
    memory,
    stabilizer,
    second_gain,
    second_gate,
    second_up,
    second_down,
):
    first = half_mlp(tokens, first_gain, first_gate, first_up, first_down)
    matrices = (
        query_weight,
        key_weight,
        value_weight,
        outgate_weight,
        ingate_weight,
        forget_weight,
    )
    block_width = query_weight.shape[0]
    gain_block = lax.dynamic_slice_in_dim(
        mix_gain, lax.axis_index("kv") * block_width, block_width, 0
    )
    mix_partials, squares = fold_columns(
        lax.all_gather(first, "tp", axis=1, tiled=True), gain_block, matrices
    )
    query_sum, key_sum, value_sum, outgate_sum, ingate_sum, forget_sum, squares = (
        lax.psum_scatter(mix_partials[0], "kv", scatter_dimension=0, tiled=True),
        lax.psum_scatter(mix_partials[1], "kv", scatter_dimension=0, tiled=True),
        lax.psum_scatter(mix_partials[2], "kv", scatter_dimension=0, tiled=True),
        lax.psum_scatter(mix_partials[3], "kv", scatter_dimension=0, tiled=True),
        lax.psum_scatter(mix_partials[4], "kv", scatter_dimension=0, tiled=True),
        lax.psum_scatter(mix_partials[5], "kv", scatter_dimension=0, tiled=True),
        lax.psum_scatter(squares, "kv", scatter_dimension=0, tiled=True),
    )
    row_factor = row_scale(squares, mix_gain.shape[0])
    seq_local, heads_local, key_width, value_width = memory.shape
    query = (row_factor * query_sum).astype(jnp.bfloat16).reshape(seq_local, heads_local, key_width)
    keys = (row_factor * key_sum).astype(jnp.bfloat16).reshape(seq_local, heads_local, key_width)
    values = (
        (row_factor * value_sum).astype(jnp.bfloat16).reshape(seq_local, heads_local, value_width)
    )
    outgate = (
        (row_factor * outgate_sum).astype(jnp.bfloat16).reshape(seq_local, heads_local, value_width)
    )
    head_start = lax.axis_index("tp") * heads_local
    ingate = lax.dynamic_slice_in_dim(row_factor * ingate_sum, head_start, heads_local, 1)
    forget = (
        lax.dynamic_slice_in_dim(row_factor * forget_sum, head_start, heads_local, 1)
        + forget_bias[None, :]
    )
    log_forget = jax.nn.log_sigmoid(forget)
    ceiling = jnp.maximum(log_forget + stabilizer, ingate)
    retain = jnp.exp(log_forget + stabilizer - ceiling)
    admission = jnp.exp(ingate - ceiling)
    scaled_keys = keys.astype(jnp.float32) * key_width ** (-0.5)
    outer_product = jnp.einsum("shd,she->shde", scaled_keys, values.astype(jnp.float32))
    memory_next = retain[..., None, None] * memory + admission[..., None, None] * outer_product
    readout = jnp.einsum(
        "shd,shde->she", query.astype(jnp.float32), memory_next, precision=lax.Precision.HIGHEST
    )
    normalized = readout * lax.rsqrt(jnp.mean(readout * readout, axis=-1, keepdims=True) + epsilon)
    gated = (
        normalized
        * head_gain.reshape(heads_local, value_width).astype(jnp.float32)
        * jax.nn.sigmoid(outgate.astype(jnp.float32))
    )
    mixed = gated.reshape(seq_local, heads_local * value_width).astype(jnp.bfloat16)
    mix_terms = jnp.dot(
        lax.all_gather(mixed, "kv", axis=0, tiled=True),
        mixout_weight,
        preferred_element_type=jnp.float32,
    )
    mix_branch = lax.psum_scatter(
        mix_terms.astype(jnp.bfloat16), "tp", scatter_dimension=1, tiled=True
    ).astype(jnp.float32)
    after_mix = (first.astype(jnp.float32) + mix_branch).astype(jnp.bfloat16)
    layer_out = half_mlp(after_mix, second_gain, second_gate, second_up, second_down)
    return (layer_out, memory_next, ceiling)


def fused_kernel(
    kv_count,
    tp_count,
    tokens,
    first_gain,
    mix_gain,
    second_gain,
    head_gain,
    forget_bias,
    stabilizer,
    first_gate,
    first_up,
    first_down,
    query_weight,
    key_weight,
    value_weight,
    outgate_weight,
    ingate_weight,
    forget_weight,
    mixout_weight,
    memory,
    second_gate,
    second_up,
    second_down,
    layer_out,
    memory_next,
    ceiling_out,
    gate_a,
    up_a,
    down_a,
    gate_b,
    up_b,
    down_b,
    query_w,
    key_w,
    value_w,
    outgate_w,
    ingate_w,
    forget_w,
    mixout_w,
    memory_v,
    gathered_a,
    parts_a,
    landed_a,
    gathered_b,
    parts_b,
    landed_b,
    first_v,
    block_v,
    proj_send,
    proj_land,
    reduced,
    readout_v,
    mixed_send,
    mixed_land,
    mixed_all,
    mix_send,
    mix_land,
    after_v,
    load_sem,
    store_sem,
    all_send,
    all_recv,
    tp_send,
    tp_recv,
    kv_send,
    kv_recv,
):
    total = kv_count * tp_count
    wide_dims = (((1,), (1,)), ((), ()))
    my_kv = lax.axis_index("kv")
    my_tp = lax.axis_index("tp")
    me = my_kv * tp_count + my_tp
    rows, chunk = tokens.shape
    block = tp_count * chunk
    model_width = total * chunk
    seq_local, heads_local, key_width, value_width = memory.shape

    loads = [
        pltpu.make_async_copy(source, target, load_sem.at[n])
        for n, (source, target) in enumerate(
            (
                (first_gate, gate_a),
                (first_up, up_a),
                (first_down, down_a),
                (query_weight, query_w),
                (key_weight, key_w),
                (value_weight, value_w),
                (outgate_weight, outgate_w),
                (ingate_weight, ingate_w),
                (forget_weight, forget_w),
                (memory, memory_v),
                (mixout_weight, mixout_w),
                (second_gate, gate_b),
                (second_up, up_b),
                (second_down, down_b),
            )
        )
    ]
    for load in loads[:3]:
        load.start()

    barrier = pltpu.get_barrier_semaphore()

    def greet(step, carry):
        peer = (me + step) % total
        pl.semaphore_signal(
            barrier,
            inc=1,
            device_id={"kv": peer // tp_count, "tp": peer % tp_count},
            device_id_type=pl.DeviceIdType.MESH,
        )
        return carry

    lax.fori_loop(1, total, greet, 0)
    pl.semaphore_wait(barrier, total - 1)

    def send(source, target, send_sem, recv_sem, kv_index, tp_index):
        return pltpu.make_async_remote_copy(
            src_ref=source,
            dst_ref=target,
            send_sem=send_sem,
            recv_sem=recv_sem,
            device_id={"kv": kv_index, "tp": tp_index},
            device_id_type=pl.DeviceIdType.MESH,
        )

    partner_tp = my_tp + 1 - 2 * (my_tp % 2)

    def twin(peer):
        return peer + 1 - 2 * (peer % 2)

    def direct(source, target, phase, peer):
        return send(
            source,
            target.at[me],
            all_send.at[phase, peer],
            all_recv.at[phase, me],
            peer // tp_count,
            peer % tp_count,
        )

    def forward(source, target, phase, peer):
        return send(
            source,
            target.at[peer],
            all_send.at[phase, twin(peer)],
            all_recv.at[phase, peer],
            my_kv,
            partner_tp,
        )

    def share_all(source, target, phase):
        def step_of(step, carry):
            direct(source, target, phase, (me + 2 * step) % total).start()
            return carry

        forward(source, target, phase, me).start()
        lax.fori_loop(1, total // 2, step_of, 0)

    def shared_all(source, target, phase):
        def step_of(step, carry):
            peer = (me + 2 * step) % total
            direct(source, target, phase, peer).wait_send()
            forward(target.at[peer], target, phase, peer).wait_send()
            return carry

        forward(source, target, phase, me).wait_send()
        lax.fori_loop(1, total // 2, step_of, 0)

    def sent_all(source, target, phase):
        def step_of(step, carry):
            peer = (me + step) % total
            direct(source.at[peer], target, phase, peer).wait_send()
            return carry

        lax.fori_loop(1, total, step_of, 0)

    def arrived(target, phase, peer):
        send(
            target.at[peer],
            target.at[peer],
            all_send.at[phase, peer],
            all_recv.at[phase, peer],
            peer // tp_count,
            peer % tp_count,
        ).wait_recv()

    def half(own, gain, gate_w, up_w, down_w, gathered, parts, landed, phase, ready):
        share_all(own, gathered, phase)
        gathered[me] = own[...]
        ready(0)
        hidden_units = gate_w.shape[0]

        def group_of(step, carry):
            gate_sum, up_sum, squares = carry
            group = (my_kv + step) % kv_count

            @pl.when(step < kv_count - 1)
            def _():
                relay((my_kv + step + 1) % kv_count)

            for pair in range(tp_count // 2):
                arrived(gathered, phase, group * tp_count + 2 * pair + 1 - my_tp % 2)

            wide = jnp.concatenate(
                [gathered[group * tp_count + t].astype(jnp.float32) for t in range(tp_count)],
                axis=1,
            )
            start = pl.multiple_of(group * block, block)
            normed = (wide * gain[pl.ds(start, block)].astype(jnp.float32)[None, :]).astype(jnp.bfloat16)
            gate_sum = gate_sum + lax.dot_general(
                normed, gate_w[:, pl.ds(start, block)], wide_dims, preferred_element_type=jnp.float32
            )
            up_sum = up_sum + lax.dot_general(
                normed, up_w[:, pl.ds(start, block)], wide_dims, preferred_element_type=jnp.float32
            )
            return gate_sum, up_sum, squares + jnp.sum(wide * wide, axis=1, keepdims=True)

        def relay(group):
            for pair in range(tp_count // 2):
                peer = group * tp_count + 2 * pair + my_tp % 2

                @pl.when(peer != me)
                def _():
                    arrived(gathered, phase, peer)
                    forward(gathered.at[peer], gathered, phase, peer).start()

        relay(my_kv)
        zero = jnp.zeros((rows, hidden_units), jnp.float32)
        gate_sum, up_sum, squares = lax.fori_loop(
            0, kv_count, group_of, (zero, zero, jnp.zeros((rows, 1), jnp.float32))
        )
        factor = lax.rsqrt(squares / model_width + epsilon)
        gate_sum = factor * gate_sum
        hidden = (gate_sum / (1.0 + jnp.exp(-gate_sum)) * (factor * up_sum)).astype(jnp.bfloat16)
        ready(1)

        def ship(group):
            for t in range(tp_count):
                peer = group * tp_count + t

                @pl.when(peer != me)
                def _():
                    direct(parts.at[peer], landed, phase + 1, peer).start()

        def down_of(step, carry):
            group = (my_kv + 1 + step) % kv_count
            start = pl.multiple_of(group * block, block)
            part = jnp.dot(
                hidden, down_w[:, pl.ds(start, block)], preferred_element_type=jnp.float32
            ).astype(jnp.bfloat16)
            for t in range(tp_count):
                parts[group * tp_count + t] = part[:, t * chunk : (t + 1) * chunk]

            @pl.when(step > 0)
            def _():
                ship((my_kv + step) % kv_count)

            return carry

        lax.fori_loop(0, kv_count, down_of, 0)
        ship(my_kv)

        def add_of(step, carry):
            peer = (me + step) % total
            arrived(landed, phase + 1, peer)
            return carry + landed[peer].astype(jnp.float32)

        branch = lax.fori_loop(1, total, add_of, parts[me].astype(jnp.float32))
        return (own[...].astype(jnp.float32) + 0.5 * branch).astype(jnp.bfloat16)

    def ready_a(stage):
        if stage == 0:
            for load in loads[3:]:
                load.start()
            loads[0].wait()
            loads[1].wait()
            proj_send[...] = jnp.zeros_like(proj_send)
            reduced[...] = jnp.zeros_like(reduced)
            readout_v[...] = jnp.zeros_like(readout_v)
        else:
            loads[2].wait()

    def ready_b(stage):
        if stage == 0:
            loads[11].wait()
            loads[12].wait()
        else:
            loads[13].wait()

    first = half(
        tokens, first_gain, gate_a, up_a, down_a, gathered_a, parts_a, landed_a, 0, ready_a
    )
    first_v[...] = first

    def tp_copy(source, target, phase, index):
        return send(
            source, target.at[my_tp], tp_send.at[phase, index], tp_recv.at[phase, my_tp], my_kv, index
        )

    def tp_arrived(target, phase, index):
        send(
            target.at[index],
            target.at[index],
            tp_send.at[phase, index],
            tp_recv.at[phase, index],
            my_kv,
            index,
        ).wait_recv()

    def kv_copy(source, target, phase, index):
        return send(
            source, target.at[my_kv], kv_send.at[phase, index], kv_recv.at[phase, my_kv], index, my_tp
        )

    def kv_arrived(target, phase, index):
        send(
            target.at[index],
            target.at[index],
            kv_send.at[phase, index],
            kv_recv.at[phase, index],
            index,
            my_tp,
        ).wait_recv()

    for step in range(1, tp_count):
        tp_copy(first_v, block_v, 0, (my_tp + step) % tp_count).start()
    block_v[my_tp] = first
    for load in loads[3:9]:
        load.wait()
    for step in range(1, tp_count):
        tp_arrived(block_v, 0, (my_tp + step) % tp_count)
    wide = jnp.concatenate([block_v[t].astype(jnp.float32) for t in range(tp_count)], axis=1)
    start = pl.multiple_of(my_kv * block, block)
    normed = (wide * mix_gain[pl.ds(start, block)].astype(jnp.float32)[None, :]).astype(jnp.bfloat16)
    offsets = [0]
    for weight in (query_w, key_w, value_w, outgate_w):
        offsets.append(offsets[-1] + weight.shape[1])
    edge = offsets[-1]
    lane = 128
    head_count = ingate_w.shape[0]
    pieces = [
        (offset, jnp.dot(normed, weight[...], preferred_element_type=jnp.float32))
        for offset, weight in zip(
            offsets, (query_w, key_w, value_w, outgate_w)
        )
    ] + [
        (
            edge + n * lane,
            lax.dot_general(normed, weight[...], wide_dims, preferred_element_type=jnp.float32),
        )
        for n, weight in enumerate((ingate_w, forget_w))
    ]
    squares = jnp.broadcast_to(jnp.sum(wide * wide, axis=1, keepdims=True), (rows, lane))
    pieces.append((edge + 2 * lane, squares))
    for k in range(kv_count):
        for offset, piece in pieces:
            proj_send[k, :, offset : offset + piece.shape[1]] = piece[
                k * seq_local : (k + 1) * seq_local, :
            ]
    for step in range(1, kv_count):
        peer = (my_kv + step) % kv_count
        kv_copy(proj_send.at[peer], proj_land, 0, peer).start()
    loads[9].wait()
    summed = proj_send[my_kv]
    for step in range(1, kv_count):
        peer = (my_kv + step) % kv_count
        kv_arrived(proj_land, 0, peer)
        summed = summed + proj_land[peer]
    reduced[0:seq_local, :] = summed
    everything = reduced[...]
    factor = lax.rsqrt(everything[:, edge + 2 * lane : edge + 2 * lane + 1] / model_width + epsilon)
    query, keys, values, outgate = [
        (factor * everything[:, offsets[n] : offsets[n + 1]]).astype(jnp.bfloat16).astype(jnp.float32)
        for n in range(4)
    ]
    ingate_sum = everything[:, edge : edge + head_count]
    forget_sum = everything[:, edge + lane : edge + lane + head_count]
    ingate = ingate_sum[:, 0:heads_local]
    forget = forget_sum[:, 0:heads_local]
    for t in range(1, tp_count):
        here = my_tp == t
        ingate = jnp.where(here, ingate_sum[:, t * heads_local : (t + 1) * heads_local], ingate)
        forget = jnp.where(here, forget_sum[:, t * heads_local : (t + 1) * heads_local], forget)
    ingate = (factor * ingate)[0:seq_local]
    forget = (factor * forget)[0:seq_local] + forget_bias[...]
    log_forget = jnp.minimum(forget, 0.0) - jnp.log1p(jnp.exp(-jnp.abs(forget)))
    diagonal = lax.broadcasted_iota(jnp.int32, (seq_local, seq_local), 0) == (
        lax.broadcasted_iota(jnp.int32, (seq_local, seq_local), 1)
    )
    head_lane = lax.broadcasted_iota(jnp.int32, (seq_local, heads_local), 1)
    scale_now = jnp.zeros((seq_local, heads_local), jnp.float32)
    for h in range(heads_local):
        column = jnp.sum(
            jnp.where(diagonal, stabilizer[h : h + 1, :], 0.0), axis=1, keepdims=True
        )
        scale_now = jnp.where(head_lane == h, column, scale_now)
    shifted = log_forget + scale_now
    ceiling = jnp.maximum(shifted, ingate)
    retain = jnp.exp(shifted - ceiling)
    admission = jnp.exp(ingate - ceiling) * key_width ** (-0.5)
    for h in range(heads_local):
        ceiling_out[h : h + 1, :] = jnp.sum(
            jnp.where(diagonal, ceiling[:, h : h + 1], 0.0), axis=0, keepdims=True
        )
    row_index = lax.broadcasted_iota(jnp.int32, (reduced.shape[0], key_width), 0)
    stores = []
    for h in range(heads_local):
        head_keys = keys[:, h * key_width : (h + 1) * key_width]
        head_values = values[:, h * value_width : (h + 1) * value_width]
        head_query = query[:, h * key_width : (h + 1) * key_width]
        for s in range(seq_local):
            outer = lax.dot_general(
                jnp.where(row_index == s, head_keys, 0.0),
                head_values,
                (((0,), (0,)), ((), ())),
                preferred_element_type=jnp.float32,
            )
            updated = (
                retain[s : s + 1, h : h + 1] * memory_v[s, h]
                + admission[s : s + 1, h : h + 1] * outer
            )
            memory_v[s, h] = updated
            read = jnp.dot(
                head_query,
                updated,
                precision=lax.Precision.HIGHEST,
                preferred_element_type=jnp.float32,
            )
            readout_v[s : s + 1, h * value_width : (h + 1) * value_width] = read[s : s + 1, :]
    store = pltpu.make_async_copy(memory_v, memory_next, store_sem)
    for h in range(heads_local):
        span = slice(h * value_width, (h + 1) * value_width)
        readout = readout_v[:, span]
        normalized = readout * lax.rsqrt(
            jnp.mean(readout * readout, axis=-1, keepdims=True) + epsilon
        )
        gated = (
            normalized * head_gain[span].astype(jnp.float32)[None, :] / (1.0 + jnp.exp(-outgate[:, span]))
        )
        mixed_send[:, span] = gated.astype(jnp.bfloat16).astype(jnp.float32)[0:seq_local, :]
    store.start()
    for step in range(1, kv_count):
        kv_copy(mixed_send, mixed_land, 1, (my_kv + step) % kv_count).start()
    mixed_land[my_kv] = mixed_send[...]
    loads[10].wait()
    for step in range(1, kv_count):
        kv_arrived(mixed_land, 1, (my_kv + step) % kv_count)
    for k in range(kv_count):
        mixed_all[k * seq_local : (k + 1) * seq_local, :] = mixed_land[k]
    mix_terms = jnp.dot(
        mixed_all[...].astype(jnp.bfloat16), mixout_w[...], preferred_element_type=jnp.float32
    ).astype(jnp.bfloat16)
    for t in range(tp_count):
        mix_send[t] = mix_terms[:, t * chunk : (t + 1) * chunk]
    for step in range(1, tp_count):
        peer = (my_tp + step) % tp_count
        tp_copy(mix_send.at[peer], mix_land, 1, peer).start()
    branch = mix_send[my_tp].astype(jnp.float32)
    for step in range(1, tp_count):
        peer = (my_tp + step) % tp_count
        tp_arrived(mix_land, 1, peer)
        branch = branch + mix_land[peer].astype(jnp.float32)
    after_v[...] = (first.astype(jnp.float32) + branch).astype(jnp.bfloat16)
    layer_out[...] = half(
        after_v, second_gain, gate_b, up_b, down_b, gathered_b, parts_b, landed_b, 2, ready_b
    )

    shared_all(tokens, gathered_a, 0)
    sent_all(parts_a, landed_a, 1)
    shared_all(after_v, gathered_b, 2)
    sent_all(parts_b, landed_b, 3)
    for step in range(1, tp_count):
        peer = (my_tp + step) % tp_count
        tp_copy(first_v, block_v, 0, peer).wait_send()
        tp_copy(mix_send.at[peer], mix_land, 1, peer).wait_send()
    for step in range(1, kv_count):
        peer = (my_kv + step) % kv_count
        kv_copy(proj_send.at[peer], proj_land, 0, peer).wait_send()
        kv_copy(mixed_send, mixed_land, 1, peer).wait_send()
    store.wait()


def fused_on_device(
    kv_count,
    tp_count,
    tokens,
    first_gain,
    first_gate,
    first_up,
    first_down,
    mix_gain,
    query_weight,
    key_weight,
    value_weight,
    outgate_weight,
    ingate_weight,
    forget_weight,
    forget_bias,
    head_gain,
    mixout_weight,
    memory,
    stabilizer,
    second_gain,
    second_gate,
    second_up,
    second_down,
):
    total = kv_count * tp_count
    rows, chunk = tokens.shape
    seq_local = memory.shape[0]
    first_gate, first_up, second_gate, second_up = (
        first_gate.T,
        first_up.T,
        second_gate.T,
        second_up.T,
    )
    ingate_weight, forget_weight = ingate_weight.T, forget_weight.T
    width = sum(w.shape[1] for w in (query_weight, key_weight, value_weight, outgate_weight)) + 384
    mixed_width = outgate_weight.shape[1]
    held_rows = max(8, seq_local)

    def like(array):
        return pltpu.VMEM(array.shape, array.dtype)

    exchange = pltpu.VMEM((total, rows, chunk), jnp.bfloat16)
    tile = pltpu.VMEM((rows, chunk), jnp.bfloat16)
    tp_tiles = pltpu.VMEM((tp_count, rows, chunk), jnp.bfloat16)
    vmem = pl.BlockSpec(memory_space=pltpu.VMEM)
    hbm = pl.BlockSpec(memory_space=pl.ANY)
    layer_out, memory_next, ceiling = pl.pallas_call(
        functools.partial(fused_kernel, kv_count, tp_count),
        out_shape=(
            jax.ShapeDtypeStruct(tokens.shape, jnp.bfloat16),
            jax.ShapeDtypeStruct(memory.shape, memory.dtype),
            jax.ShapeDtypeStruct(stabilizer.shape[::-1], stabilizer.dtype),
        ),
        in_specs=[vmem] * 7 + [hbm] * 14,
        out_specs=(vmem, hbm, vmem),
        scratch_shapes=[
            like(first_gate),
            like(first_up),
            like(first_down),
            like(second_gate),
            like(second_up),
            like(second_down),
            like(query_weight),
            like(key_weight),
            like(value_weight),
            like(outgate_weight),
            like(ingate_weight),
            like(forget_weight),
            like(mixout_weight),
            like(memory),
            exchange,
            exchange,
            exchange,
            exchange,
            exchange,
            exchange,
            tile,
            tp_tiles,
            pltpu.VMEM((kv_count, seq_local, width), jnp.float32),
            pltpu.VMEM((kv_count, seq_local, width), jnp.float32),
            pltpu.VMEM((held_rows, width), jnp.float32),
            pltpu.VMEM((held_rows, mixed_width), jnp.float32),
            pltpu.VMEM((seq_local, mixed_width), jnp.float32),
            pltpu.VMEM((kv_count, seq_local, mixed_width), jnp.float32),
            pltpu.VMEM((rows, mixed_width), jnp.float32),
            tp_tiles,
            tp_tiles,
            tile,
            pltpu.SemaphoreType.DMA((14,)),
            pltpu.SemaphoreType.DMA,
            pltpu.SemaphoreType.DMA((4, total)),
            pltpu.SemaphoreType.DMA((4, total)),
            pltpu.SemaphoreType.DMA((2, tp_count)),
            pltpu.SemaphoreType.DMA((2, tp_count)),
            pltpu.SemaphoreType.DMA((2, kv_count)),
            pltpu.SemaphoreType.DMA((2, kv_count)),
        ],
        compiler_params=pltpu.CompilerParams(
            collective_id=0, has_side_effects=True, vmem_limit_bytes=60 * 1024 * 1024
        ),
    )(
        tokens,
        first_gain,
        mix_gain,
        second_gain,
        head_gain,
        forget_bias[None, :],
        stabilizer.T,
        first_gate,
        first_up,
        first_down,
        query_weight,
        key_weight,
        value_weight,
        outgate_weight,
        ingate_weight,
        forget_weight,
        mixout_weight,
        memory,
        second_gate,
        second_up,
        second_down,
    )
    return layer_out, memory_next, ceiling.T


def choose(kv_count, tp_count, *arrays):
    if arrays[0].shape[1] % 128 == 0 and tp_count % 2 == 0:
        return fused_on_device(kv_count, tp_count, *arrays)
    return on_device(*arrays)


def solution(mesh):
    in_specs = (
        P(None, ("kv", "tp")),
        P(),
        P(None, ("kv", "tp")),
        P(None, ("kv", "tp")),
        P(("kv", "tp"), None),
        P(),
        P("kv", "tp"),
        P("kv", "tp"),
        P("kv", "tp"),
        P("kv", "tp"),
        P("kv", None),
        P("kv", None),
        P("tp"),
        P("tp"),
        P("tp", "kv"),
        P("kv", "tp", None, None),
        P("kv", "tp"),
        P(),
        P(None, ("kv", "tp")),
        P(None, ("kv", "tp")),
        P(("kv", "tp"), None),
    )
    out_specs = (P(None, ("kv", "tp")), P("kv", "tp", None, None), P("kv", "tp"))
    return jax.shard_map(
        functools.partial(choose, mesh.shape["kv"], mesh.shape["tp"]),
        mesh=mesh,
        in_specs=in_specs, out_specs=out_specs, check_vma=False
    )
```
